32 devices in a mesh: row: 4 (over z), col: 8 (over y, x, core).
Axes of the slice: x: 2, y: 2, z: 4, core: 2. Of those that a mesh axis runs over, the one named last changes fastest.
Arguments:
- tokens: bfloat16 [32, 144, 2048], P('row', 'col'), may hold values from -6 to 6
- norm_gain: bfloat16 [2048], replicated, may hold values from 0.099609375 to 1.8984375
- w_in: bfloat16 [2048, 1152], replicated, may hold values from -0.125 to 0.125
- w_out: bfloat16 [1152, 2048], replicated, may hold values from -0.1875 to 0.1875
Outputs:
- mixed: bfloat16 [144, 32, 2048], P('row', 'col')
The draws below stay inside these ranges and needn't reach their ends.
All inputs are finite; a program needn't handle non-finite values.
Results may differ from the reference program's by a relative error of at most 0.013.
Values may be sent and summed in bfloat16 or wider, within the bound.
A program may use at most 64 MiB of HBM per device.

```python
import jax
import jax.numpy as jnp
from jax import lax

D = 2048
GROUP = 128
F = 1152
LEN_A = 32
LEN_B = 144
N_COL = 8


def level_of(stream_key, dims, cuts, low, high):
    level = 1.0
    for axis_at, parts in cuts:
        draws = jax.random.uniform(jax.random.fold_in(jax.random.fold_in(stream_key, 6), axis_at), (parts,), jnp.float32, low / len(cuts), high / len(cuts))
        level = level * jnp.repeat(jnp.exp(draws), dims[axis_at] // parts).reshape((-1,) + (1,) * (len(dims) - 1 - axis_at))
    return level


def gaussian(stream_key, dims, scale, bound, cuts=(), kind=jnp.bfloat16):
    array = scale * jax.random.normal(stream_key, dims, jnp.float32)
    if cuts:
        array = array * level_of(stream_key, dims, cuts, -0.22, 0.18)
    return jnp.clip(array, -bound, bound).astype(kind)


def setup_inputs(seed: int = 0) -> dict:
    arg_keys = jax.random.split(jax.random.key(seed), 5)
    tokens = gaussian(arg_keys[0], (LEN_A, LEN_B, D), 1.0, 6.0, ((0, 4), (1, 8)))
    norm_gain = jnp.clip(1.0 + 0.18 * jax.random.normal(arg_keys[1], (D,), jnp.float32), 0.099609375, 1.8984375).astype(jnp.bfloat16)
    w_in = gaussian(arg_keys[2], (D, F), D ** -0.5, 0.125)
    w_out = gaussian(arg_keys[3], (F, D), F ** -0.5, 0.1875)
    return dict(tokens=tokens, norm_gain=norm_gain, w_in=w_in, w_out=w_out)


norm_eps = 1e-06

def folded_order(length_first, devices):
    block = length_first // devices
    half_block = block // 2
    series = jnp.arange(length_first, dtype=jnp.int32)
    device = series // block
    inner = series % block
    lower = device * half_block + inner
    upper = length_first - device * half_block - (inner - half_block)
    upper = jnp.where((device == 0) & (inner == half_block), length_first // 2, upper)
    return (jnp.where(inner < half_block, lower, upper) % length_first).astype(jnp.int32)

def reference(tokens, norm_gain, w_in, w_out):
    length_first, length_second, features = tokens.shape
    positions = length_first * length_second
    floats = tokens.astype(jnp.float32).reshape(positions, features)
    normed = (floats * lax.rsqrt(lax.optimization_barrier(jnp.mean(floats * floats, axis=-1, keepdims=True)) + norm_eps) * norm_gain.astype(jnp.float32)).astype(jnp.bfloat16)
    mapped = jnp.dot(normed, w_in, preferred_element_type=jnp.float32).astype(jnp.bfloat16)
    channels = mapped.shape[1]
    grouped = mapped.astype(jnp.float32).reshape(positions, channels // GROUP, GROUP).transpose(1, 0, 2)

    def one_group(block):
        return jnp.fft.fft2(block, norm='ortho').real.astype(jnp.float32)
    spectrum = lax.map(one_group, grouped).transpose(1, 0, 2).reshape(positions, channels)
    spectrum = spectrum.astype(jnp.bfloat16)
    mixed = jnp.dot(spectrum, w_out, preferred_element_type=jnp.float32).astype(jnp.bfloat16)
    mixed = mixed.reshape(length_second, length_first, features)
    return jnp.take(mixed, folded_order(length_first, N_COL), axis=1)
```

```python
import functools
import math

import jax
import jax.numpy as jnp
import numpy as np
from jax import lax
from jax.experimental import pallas as pl
from jax.experimental.pallas import tpu as pltpu
from jax.sharding import PartitionSpec as P

GROUP = 128
LANES = 128
MESH = pl.DeviceIdType.MESH


norm_eps = 1e-06
highest = lax.Precision.HIGHEST


def folded_list(length_first, devices):
    block = length_first // devices
    half = block // 2
    result = np.zeros(length_first, np.int64)
    for device in range(devices):
        for inner in range(block):
            if inner < half:
                value = device * half + inner
            elif device == 0 and inner == half:
                value = length_first // 2
            else:
                value = length_first - device * half - (inner - half)
            result[device * block + inner] = value % length_first
    return result


def channel_tables(row_count):
    width = GROUP // row_count
    half = width // 2
    per_tile = LANES // width
    j = np.arange(GROUP)
    forward = np.zeros((row_count, per_tile * GROUP, LANES))
    back = np.zeros((row_count, LANES, per_tile * GROUP))
    for row in range(row_count):
        for x in range(width):
            m = row * half + x % half
            cosine = x < half
            column = np.cos(2 * np.pi * j * m / GROUP) if cosine else np.sin(2 * np.pi * j * m / GROUP)
            entries = [(m, 1.0)]
            if not cosine and m == 0:
                column = np.cos(np.pi * j)
                entries = [(GROUP // 2, 1.0)]
            elif m:
                entries = [(m, 1.0 if cosine else -1.0), (GROUP - m, 1.0)]
            for g in range(per_tile):
                forward[row, g * GROUP : (g + 1) * GROUP, g * width + x] = column
                for at, sign in entries:
                    back[row, g * width + x, g * GROUP + at] = sign
    return forward, back


def position_tables(rows_first, rows_second, row_count, col_count, padded):
    length_first = rows_first * row_count
    length_second = rows_second * col_count
    positions = length_first * length_second
    block = length_first // col_count
    half = block // 2
    a = np.arange(length_first)
    first = np.zeros((col_count, col_count, padded, length_first, rows_second))
    for col in range(col_count):
        for i in range(rows_second):
            p = a * length_second + col * rows_second + i
            for target in range(col_count):
                for f_at in range(half):
                    f = target * half + f_at
                    re_at, im_at = (2 * f_at) * rows_second + i, (2 * f_at + 1) * rows_second + i
                    if f == 0:
                        first[col, target, re_at, :, i] = 1.0
                        first[col, target, im_at, :, i] = (-1.0) ** a
                    else:
                        angle = 2 * np.pi * (f * p % positions) / positions
                        first[col, target, re_at, :, i] = np.cos(angle)
                        first[col, target, im_at, :, i] = -np.sin(angle)
    first = first.reshape(col_count, col_count * padded, length_first * rows_second)
    k_b = np.arange(length_second)
    second = np.zeros((2, 2, length_second, block, col_count, padded))
    for other in range(2):
        for s in range(block):
            for source in range(col_count):
                for i in range(rows_second):
                    b = source * rows_second + i
                    f_at, upper = s % half, s >= half
                    re_at, im_at = (2 * f_at) * rows_second + i, (2 * f_at + 1) * rows_second + i
                    if other == 0 and f_at == 0:
                        shift = length_first // 2 if upper else 0
                        angle = 2 * np.pi * (b * (k_b * length_first + shift) % positions) / positions
                        at = im_at if upper else re_at
                        second[other, 0, :, s, source, at] = np.cos(angle)
                        second[other, 1, :, s, source, at] = np.sin(angle)
                        continue
                    sign = -1.0 if upper else 1.0
                    angle = 2 * np.pi * (b * (k_b + (1 if upper else 0)) % length_second) / length_second
                    second[other, 0, :, s, source, re_at] = np.cos(angle)
                    second[other, 0, :, s, source, im_at] = np.sin(angle) * sign
                    second[other, 1, :, s, source, re_at] = np.sin(angle)
                    second[other, 1, :, s, source, im_at] = -np.cos(angle) * sign
    second = second.reshape(2, 2, length_second * block, col_count * padded)
    return first, second / math.sqrt(positions * GROUP)


def kernel(
    n_r, n_c, tokens, gain, w_in, w_out, forward, first, second, back, out,
    tok_v, rows_v, norm_v, win_v, wout_v, forward_v, first_v, second_v, back_v,
    sent1, came1, sent2, came2, sent3, came3, spec_v,
    load_sem, self_sem, send_sem1, recv_sem1, send_sem2, recv_sem2, send_sem3, recv_sem3,
):
    row, col = lax.axis_index("row"), lax.axis_index("col")
    rows_first, rows_second, features = tokens.shape
    channels = w_in.shape[1]
    tiles = sent1.shape[0]
    span = n_r * GROUP

    barrier = pltpu.get_barrier_semaphore()
    for d in range(1, n_r):
        pl.semaphore_signal(barrier, inc=1, device_id={"row": lax.rem(row + d, n_r)}, device_id_type=MESH)
    for d in range(1, n_c):
        pl.semaphore_signal(barrier, inc=1, device_id={"col": lax.rem(col + d, n_c)}, device_id_type=MESH)

    spans = [(t * span, min(channels, (t + 1) * span)) for t in range(tiles)]
    load_tok = pltpu.make_async_copy(tokens, tok_v, load_sem.at[0])
    load_tok.start()
    load_win = []
    for t, (lo, hi) in enumerate(spans):
        load_win.append(
            pltpu.make_async_copy(w_in.at[:, lo:hi], win_v.at[:, lo:hi], load_sem.at[6 + t])
        )
    load_forward = pltpu.make_async_copy(forward, forward_v, load_sem.at[1])
    load_first = pltpu.make_async_copy(first.at[col], first_v, load_sem.at[2])
    load_second = pltpu.make_async_copy(second.at[jnp.minimum(col, 1)], second_v, load_sem.at[3])
    load_back = pltpu.make_async_copy(back, back_v, load_sem.at[4])
    load_wout = pltpu.make_async_copy(w_out, wout_v, load_sem.at[5])
    load_win[0].start()
    load_forward.start()
    for copy in load_win[1:]:
        copy.start()
    load_first.start()
    load_second.start()

    load_tok.wait()
    for a in range(rows_first):
        rows_v[a * rows_second : (a + 1) * rows_second, :] = tok_v[a].astype(jnp.float32)
    floats = rows_v[...]
    inverse = lax.rsqrt(jnp.mean(floats * floats, axis=-1, keepdims=True) + norm_eps)
    norm_v[...] = (floats * inverse * gain[...].astype(jnp.float32)).astype(jnp.bfloat16)

    def exchange(sent, came, send_sem, recv_sem, self_sem_at, t, me, count, axis):
        own = pltpu.make_async_copy(sent.at[t, me], came.at[t, me], self_sem_at)
        own.start()
        copies = [own]
        for d in range(1, count):
            target = lax.rem(me + d, count)
            copy = pltpu.make_async_remote_copy(
                src_ref=sent.at[t, target],
                dst_ref=came.at[t, me],
                send_sem=send_sem.at[t, d],
                recv_sem=recv_sem.at[t, d],
                device_id={axis: target},
                device_id_type=MESH,
            )
            copy.start()
            copies.append(copy)
        return copies

    steps1, steps2, steps3 = [], [], []
    for t, (lo, hi) in enumerate(spans):
        load_win[t].wait()
        if t == 0:
            load_forward.wait()
        mapped = jnp.dot(norm_v[...], win_v[:, lo:hi], preferred_element_type=jnp.float32).astype(jnp.bfloat16)
        for r in range(n_r):
            piece = jnp.dot(mapped, forward_v[r, : hi - lo, :], preferred_element_type=jnp.float32)
            sent1[t, r] = piece.astype(jnp.bfloat16)
        if t == 0:
            pl.semaphore_wait(barrier, n_r + n_c - 2)
        steps1.append(exchange(sent1, came1, send_sem1, recv_sem1, self_sem.at[0, t], t, row, n_r, "row"))

    load_back.start()
    load_wout.start()
    load_first.wait()
    for t in range(tiles):
        for copy in steps1[t]:
            copy.wait()
        values = came1[t].reshape(-1, LANES)
        turned = jnp.dot(first_v[...], values, preferred_element_type=jnp.float32)
        sent2[t] = turned.astype(jnp.bfloat16).reshape(sent2.shape[1:])
        steps2.append(exchange(sent2, came2, send_sem2, recv_sem2, self_sem.at[1, t], t, col, n_c, "col"))

    width = GROUP // n_r
    lane = lax.broadcasted_iota(jnp.int32, (1, LANES), 1) % width
    cosine = (lane < width // 2) | ((lane == width // 2) & (row == 0))
    load_second.wait()
    for t in range(tiles):
        for copy in steps2[t]:
            copy.wait()
        values = came2[t].reshape(-1, LANES)
        even = jnp.dot(second_v[0], values, preferred_element_type=jnp.float32)
        odd = jnp.dot(second_v[1], values, preferred_element_type=jnp.float32)
        both = jnp.where(cosine, even, odd)
        sent3[t] = both.astype(jnp.bfloat16).reshape(sent3.shape[1:])
        steps3.append(exchange(sent3, came3, send_sem3, recv_sem3, self_sem.at[2, t], t, row, n_r, "row"))

    load_back.wait()
    for t, (lo, hi) in enumerate(spans):
        for copy in steps3[t]:
            copy.wait()
        total = jnp.dot(came3[t, 0], back_v[0, :, : hi - lo], preferred_element_type=jnp.float32)
        for r in range(1, n_r):
            total = total + jnp.dot(came3[t, r], back_v[r, :, : hi - lo], preferred_element_type=jnp.float32)
        spec_v[:, lo:hi] = total.astype(jnp.bfloat16)
    load_wout.wait()
    out[...] = jnp.dot(spec_v[...], wout_v[...], preferred_element_type=jnp.float32).astype(jnp.bfloat16)


def fused_shards(n_r, n_c, tokens, norm_gain, w_in, w_out):
    rows_first, rows_second, features = tokens.shape
    channels = w_in.shape[1]
    length_first = rows_first * n_r
    block = length_first // n_c
    padded = -(-block * rows_second // 16) * 16
    groups = channels // GROUP
    tiles = -(-groups // n_r)
    rows = rows_first * rows_second
    length_second = rows_second * n_c
    out_rows = length_second // n_r * block
    forward, back = channel_tables(n_r)
    first, second = position_tables(rows_first, rows_second, n_r, n_c, padded)
    kind = jnp.bfloat16
    tables = [jnp.asarray(np.asarray(x, np.float32).astype(kind)) for x in (forward, first, second, back)]
    anywhere = pl.BlockSpec(memory_space=pl.ANY)
    vmem = pl.BlockSpec(memory_space=pltpu.VMEM)
    dma = pltpu.SemaphoreType.DMA
    out = pl.pallas_call(
        functools.partial(kernel, n_r, n_c),
        out_shape=jax.ShapeDtypeStruct((out_rows, features), kind),
        in_specs=[anywhere, vmem] + [anywhere] * 6,
        out_specs=vmem,
        scratch_shapes=[
            pltpu.VMEM(tokens.shape, kind),
            pltpu.VMEM((rows, features), jnp.float32),
            pltpu.VMEM((rows, features), kind),
            pltpu.VMEM(w_in.shape, kind),
            pltpu.VMEM(w_out.shape, kind),
            pltpu.VMEM(forward.shape, kind),
            pltpu.VMEM(first.shape[1:], kind),
            pltpu.VMEM(second.shape[1:], kind),
            pltpu.VMEM(back.shape, kind),
            pltpu.VMEM((tiles, n_r, rows, LANES), kind),
            pltpu.VMEM((tiles, n_r, rows, LANES), kind),
            pltpu.VMEM((tiles, n_c, padded, LANES), kind),
            pltpu.VMEM((tiles, n_c, padded, LANES), kind),
            pltpu.VMEM((tiles, n_r, out_rows, LANES), kind),
            pltpu.VMEM((tiles, n_r, out_rows, LANES), kind),
            pltpu.VMEM((out_rows, channels), kind),
            dma((6 + tiles,)),
            dma((3, tiles)),
            dma((tiles, n_r)),
            dma((tiles, n_r)),
            dma((tiles, n_c)),
            dma((tiles, n_c)),
            dma((tiles, n_r)),
            dma((tiles, n_r)),
        ],
        compiler_params=pltpu.CompilerParams(
            collective_id=0, has_side_effects=True, vmem_limit_bytes=60 * 1024 * 1024
        ),
    )(tokens, norm_gain.reshape(1, -1), w_in, w_out, *tables)
    return out.reshape(length_second // n_r, block, features)


def fits(n_r, n_c, tokens_shape, channels):
    length_first, length_second, _ = tokens_shape
    rows = length_first // n_r * (length_second // n_c)
    out_rows = length_second // n_r * (length_first // n_c)
    return (
        GROUP % (2 * n_r) == 0
        and length_first % (2 * n_c) == 0
        and rows % 16 == 0
        and out_rows % 16 == 0
        and length_second % n_r == 0
    )


def tables(length):
    series = jnp.arange(length, dtype=jnp.int32)
    product = series[:, None] * series[None, :] % length
    angles = product.astype(jnp.float32) * (2.0 * math.pi / length)
    return (jnp.cos(angles), jnp.sin(angles))


def folded_order(length_first, devices):
    block = length_first // devices
    half_block = block // 2
    series = jnp.arange(length_first, dtype=jnp.int32)
    device = series // block
    inner = series % block
    lower = device * half_block + inner
    upper = length_first - device * half_block - (inner - half_block)
    upper = jnp.where((device == 0) & (inner == half_block), length_first // 2, upper)
    return jnp.where(inner < half_block, lower, upper) % length_first


def to_channels(values, row_count):
    rows_first, rows_second, channels = values.shape
    width = channels // row_count
    parted = values.reshape(rows_first, rows_second, row_count, width).transpose(2, 0, 1, 3)
    return parted.reshape(row_count * rows_first, rows_second * width)


def product(table, values):
    return jnp.dot(table, values, precision=highest)


def middle(real_part, imag_part, width):
    length_first = real_part.shape[0]
    rows_second = real_part.shape[1] // width
    col_count = lax.axis_size("col")
    length_second = rows_second * col_count
    positions = length_first * length_second
    frequency = folded_order(length_first, col_count)
    series = jnp.arange(length_first, dtype=jnp.int32)
    first_angle = (frequency[:, None] * series[None, :] % length_first).astype(jnp.float32)
    first_angle = first_angle * (2.0 * math.pi / length_first)
    first_cos = jnp.cos(first_angle)
    first_sin = jnp.sin(first_angle)
    first_real = product(first_cos, real_part)
    first_imag = -product(first_sin, real_part)
    first_real = first_real + product(first_sin, imag_part)
    first_imag = first_imag + product(first_cos, imag_part)
    first_real = first_real.reshape(length_first, rows_second, width)
    first_imag = first_imag.reshape(length_first, rows_second, width)
    second_index = lax.axis_index("col") * rows_second + jnp.arange(rows_second, dtype=jnp.int32)
    twiddle_angle = (frequency[:, None] * second_index[None, :] % positions).astype(jnp.float32)
    twiddle_angle = twiddle_angle * (2.0 * math.pi / positions)
    twiddle_cos = jnp.cos(twiddle_angle)[:, :, None]
    twiddle_sin = jnp.sin(twiddle_angle)[:, :, None]
    turned_real = first_real * twiddle_cos + first_imag * twiddle_sin
    turned_imag = first_imag * twiddle_cos - first_real * twiddle_sin
    turned = jnp.stack([turned_real, turned_imag]).transpose(0, 2, 1, 3)
    turned = turned.reshape(2, rows_second, length_first * width)
    exchanged = lax.all_to_all(
        turned.astype(jnp.bfloat16), "col", split_axis=2, concat_axis=1, tiled=True
    ).astype(turned.dtype)
    second_cos, second_sin = tables(length_second)
    block = length_first // col_count
    out_shape = (length_second, block, width)
    out_real = (product(second_cos, exchanged[0]) + product(second_sin, exchanged[1])).reshape(
        out_shape
    )
    return out_real


def shards(tokens, norm_gain, w_in, w_out):
    rows_first, rows_second, features = tokens.shape
    row_count = lax.axis_size("row")
    length_first = rows_first * row_count
    length_second = rows_second * lax.axis_size("col")
    channels = w_in.shape[1]
    width = channels // row_count
    groups = channels // GROUP
    scaling = 1.0 / math.sqrt(length_first * length_second * GROUP)
    floats = tokens.astype(jnp.float32)
    normed = (
        floats
        * lax.rsqrt(jnp.mean(floats * floats, axis=-1, keepdims=True) + norm_eps)
        * norm_gain.astype(jnp.float32)
    ).astype(jnp.bfloat16)
    mapped = jnp.dot(normed.reshape(-1, features), w_in, preferred_element_type=jnp.float32)
    mapped = mapped.astype(jnp.bfloat16).reshape(rows_first, rows_second, channels)
    channel_cos, channel_sin = tables(GROUP)
    grouped = mapped.astype(jnp.float32).reshape(rows_first, rows_second, groups, GROUP)
    spec_real = jnp.einsum("abgj,jm->abgm", grouped, channel_cos, precision=highest)
    spec_imag = -jnp.einsum("abgj,jm->abgm", grouped, channel_sin, precision=highest)
    stacked = jnp.stack(
        [
            to_channels(spec_real.reshape(rows_first, rows_second, channels), row_count),
            to_channels(spec_imag.reshape(rows_first, rows_second, channels), row_count),
        ]
    )
    arrived = lax.all_to_all(
        stacked.astype(jnp.bfloat16), "row", split_axis=1, concat_axis=1, tiled=True
    ).astype(stacked.dtype)
    result = middle(arrived[0], arrived[1], width)
    spectrum = (result * scaling).astype(jnp.bfloat16)
    returned = lax.all_to_all(spectrum, "row", split_axis=0, concat_axis=2, tiled=True)
    mixed = jnp.dot(returned.reshape(-1, channels), w_out, preferred_element_type=jnp.float32)
    return mixed.astype(jnp.bfloat16).reshape(returned.shape[0], returned.shape[1], features)


def solution(mesh):
    in_specs = (P("row", "col", None), P(), P(), P())
    out_specs = P("row", "col", None)
    n_r, n_c = mesh.shape["row"], mesh.shape["col"]

    def run(tokens, norm_gain, w_in, w_out):
        whole = fits(n_r, n_c, tokens.shape, w_in.shape[1])
        body = functools.partial(fused_shards, n_r, n_c) if whole else shards
        return jax.shard_map(body, mesh=mesh, in_specs=in_specs, out_specs=out_specs, check_vma=False)(
            tokens, norm_gain, w_in, w_out
        )

    return run
```

```python
import functools
import math

import jax
import jax.numpy as jnp
import numpy as np
from jax import lax
from jax.experimental import pallas as pl
from jax.experimental.pallas import tpu as pltpu
from jax.sharding import PartitionSpec as P

GROUP = 128
LANES = 128
SUBLANES = 16
MESH = pl.DeviceIdType.MESH


norm_eps = 1e-06
highest = lax.Precision.HIGHEST


def folded_list(length_first, devices):
    block = length_first // devices
    half = block // 2
    result = np.zeros(length_first, np.int64)
    for device in range(devices):
        for inner in range(block):
            if inner < half:
                value = device * half + inner
            elif device == 0 and inner == half:
                value = length_first // 2
            else:
                value = length_first - device * half - (inner - half)
            result[device * block + inner] = value % length_first
    return result


def channel_tables(row_count):
    width = GROUP // row_count
    half = width // 2
    per_tile = LANES // width
    j = np.arange(GROUP)
    forward = np.zeros((row_count, per_tile * GROUP, LANES))
    back = np.zeros((row_count, LANES, per_tile * GROUP))
    for row in range(row_count):
        for x in range(width):
            m = row * half + x % half
            cosine = x < half
            column = np.cos(2 * np.pi * j * m / GROUP) if cosine else np.sin(2 * np.pi * j * m / GROUP)
            entries = [(m, 1.0)]
            if not cosine and m == 0:
                column = np.cos(np.pi * j)
                entries = [(GROUP // 2, 1.0)]
            elif m:
                entries = [(m, 1.0 if cosine else -1.0), (GROUP - m, 1.0)]
            for g in range(per_tile):
                forward[row, g * GROUP : (g + 1) * GROUP, g * width + x] = column
                for at, sign in entries:
                    back[row, g * width + x, g * GROUP + at] = sign
    return forward, back


def position_tables(rows_first, rows_second, row_count, col_count, chunk, chunks):
    length_first = rows_first * row_count
    length_second = rows_second * col_count
    positions = length_first * length_second
    block = length_first // col_count
    half = block // 2
    a = np.arange(length_first)
    first = np.zeros((col_count, chunks, col_count, block, chunk, row_count, chunk, rows_first))
    for col in range(col_count):
        for i in range(rows_second):
            at, j = divmod(i, chunk)
            p = a * length_second + col * rows_second + i
            for target in range(col_count):
                for f_at in range(half):
                    f = target * half + f_at
                    angle = 2 * np.pi * (f * p % positions) / positions
                    real, imag = np.cos(angle), -np.sin(angle)
                    if f == 0:
                        real, imag = np.ones(length_first), (-1.0) ** a
                    first[col, at, target, 2 * f_at, j, :, j, :] = real.reshape(row_count, rows_first)
                    first[col, at, target, 2 * f_at + 1, j, :, j, :] = imag.reshape(row_count, rows_first)
    first = first.reshape(col_count, chunks, col_count * block * chunk, row_count, chunk * rows_first)
    rest = rows_second - (chunks - 1) * chunk
    last = first[:, -1, :, :, : rest * rows_first].reshape(col_count, col_count * block * chunk, -1)
    first = first.reshape(col_count, chunks, col_count * block * chunk, -1)
    first[:, -1] = 0.0
    first[:, -1, :, : last.shape[-1]] = last
    k_b = np.arange(length_second)
    second = np.zeros((2, 2, length_second, block, col_count, chunks, block, chunk))
    for other in range(2):
        for s in range(block):
            for source in range(col_count):
                for i in range(rows_second):
                    b = source * rows_second + i
                    f_at, upper = s % half, s >= half
                    at, j = divmod(i, chunk)
                    re_at, im_at = (source, at, 2 * f_at, j), (source, at, 2 * f_at + 1, j)
                    if other == 0 and f_at == 0:
                        shift = length_first // 2 if upper else 0
                        angle = 2 * np.pi * (b * (k_b * length_first + shift) % positions) / positions
                        place = im_at if upper else re_at
                        second[(other, 0, slice(None), s) + place] = np.cos(angle)
                        second[(other, 1, slice(None), s) + place] = np.sin(angle)
                        continue
                    sign = -1.0 if upper else 1.0
                    angle = 2 * np.pi * (b * (k_b + (1 if upper else 0)) % length_second) / length_second
                    second[(other, 0, slice(None), s) + re_at] = np.cos(angle)
                    second[(other, 0, slice(None), s) + im_at] = np.sin(angle) * sign
                    second[(other, 1, slice(None), s) + re_at] = np.sin(angle)
                    second[(other, 1, slice(None), s) + im_at] = -np.cos(angle) * sign
    second = second.reshape(2, 2, length_second * block, col_count * chunks * block * chunk)
    return first, second / math.sqrt(positions * GROUP)


def widened(packed, parts, used):
    count, rows, lanes = packed.shape
    flat = packed.reshape(count * rows, lanes).astype(jnp.float32)
    keep = lax.broadcasted_iota(jnp.int32, (1, lanes), 1) < used
    blocks = []
    for p in range(parts):
        block = flat if p == 0 else pltpu.roll(flat, lanes - p * used, 1)
        blocks.append(jnp.where(keep, block, 0.0).astype(packed.dtype).reshape(count, rows, lanes))
    return blocks


def packed_rows(values, parts, used):
    rows = values.shape[0] // parts
    total = values[:rows]
    for p in range(1, parts):
        total = total + pltpu.roll(values[p * rows : (p + 1) * rows], p * used, 1)
    return total


def kernel(
    n_r, n_c, parts, tokens, gain, w_in, w_out, forward, first, second, back, out,
    tok_v, norm_v, win_v, wout_v, forward_v, first_v, second_v, back_v,
    sent1, came1, sent2, came2, sent3, came3, wide_v, wide3_v, acc_v,
    load_sem, self_sem, send_sem1, recv_sem1, send_sem2, recv_sem2, send_sem3, recv_sem3,
):
    row, col = lax.axis_index("row"), lax.axis_index("col")
    rows, features = tokens.shape
    channels = w_in.shape[1]
    tiles = sent1.shape[0]
    span = n_r * GROUP
    spans = [(t * span, min(channels, (t + 1) * span)) for t in range(tiles)]
    width = GROUP // n_r
    used = (spans[-1][1] - spans[-1][0]) // GROUP * width
    order = [tiles - 1] + list(range(tiles - 1))

    barrier = pltpu.get_barrier_semaphore()
    for d in range(1, n_r):
        pl.semaphore_signal(barrier, inc=1, device_id={"row": lax.rem(row + d, n_r)}, device_id_type=MESH)
    for d in range(1, n_c):
        pl.semaphore_signal(barrier, inc=1, device_id={"col": lax.rem(col + d, n_c)}, device_id_type=MESH)

    load_tok = pltpu.make_async_copy(tokens, tok_v, load_sem.at[0])
    load_tok.start()
    load_win = [
        pltpu.make_async_copy(w_in.at[:, lo:hi], win_v.at[:, lo:hi], load_sem.at[6 + t])
        for t, (lo, hi) in enumerate(spans)
    ]
    load_forward = pltpu.make_async_copy(forward, forward_v, load_sem.at[1])
    load_first = pltpu.make_async_copy(first.at[col], first_v, load_sem.at[2])
    load_second = pltpu.make_async_copy(second.at[jnp.minimum(col, 1)], second_v, load_sem.at[3])
    load_back = pltpu.make_async_copy(back, back_v, load_sem.at[4])
    load_wout = pltpu.make_async_copy(w_out, wout_v, load_sem.at[5])
    load_win[order[0]].start()
    load_forward.start()
    for t in order[1:]:
        load_win[t].start()
    load_first.start()
    load_second.start()

    load_tok.wait()
    floats = tok_v[...].astype(jnp.float32)
    inverse = lax.rsqrt(jnp.mean(floats * floats, axis=-1, keepdims=True) + norm_eps)
    gains = gain[...].astype(jnp.float32)
    for at in range(features // LANES):
        lanes = slice(at * LANES, (at + 1) * LANES)
        scaled = tok_v[:, lanes].astype(jnp.float32) * inverse * gains[at : at + 1, :]
        norm_v[:, lanes] = scaled.astype(jnp.bfloat16)

    def exchange(sent, came, send_sem, recv_sem, self_sem_at, t, me, count, axis):
        size = sent.shape[2]
        if axis == "row" and t == tiles - 1:
            size = size // parts
        own = pltpu.make_async_copy(sent.at[t, me, 0:size], came.at[t, me, 0:size], self_sem_at)
        copies = []
        for d in sorted(range(1, count), key=lambda d: -min(d, count - d)):
            target = lax.rem(me + d, count)
            copy = pltpu.make_async_remote_copy(
                src_ref=sent.at[t, target, 0:size],
                dst_ref=came.at[t, me, 0:size],
                send_sem=send_sem.at[t, d],
                recv_sem=recv_sem.at[t, d],
                device_id={axis: target},
                device_id_type=MESH,
            )
            copy.start()
            copies.append(copy)
        own.start()
        return [own] + copies

    steps1, steps2, steps3 = {}, {}, {}
    for t in order:
        lo, hi = spans[t]
        load_win[t].wait()
        mapped = jnp.dot(norm_v[...], win_v[:, lo:hi], preferred_element_type=jnp.float32).astype(jnp.bfloat16)
        if t == order[0]:
            load_forward.wait()
        for r in range(n_r):
            piece = jnp.dot(mapped, forward_v[r, : hi - lo, :], preferred_element_type=jnp.float32)
            if t == tiles - 1:
                sent1[t, r, 0 : rows // parts] = packed_rows(piece, parts, used).astype(jnp.bfloat16)
            else:
                sent1[t, r] = piece.astype(jnp.bfloat16)
        if t == order[0]:
            pl.semaphore_wait(barrier, n_r + n_c - 2)
        steps1[t] = exchange(sent1, came1, send_sem1, recv_sem1, self_sem.at[0, t], t, row, n_r, "row")

    load_back.start()
    load_wout.start()
    load_first.wait()
    chunks, high, depth = first_v.shape
    step = depth // n_r
    height = high // n_c
    for t in order:
        for copy in steps1[t]:
            copy.wait()
        source = came1.at[t]
        if t == tiles - 1:
            size = rows // parts
            for p, block in enumerate(widened(came1[t, :, 0:size], parts, used)):
                wide_v[:, p * size : (p + 1) * size] = block
            source = wide_v
        for at in range(chunks):
            values = source[:, at * step : min(rows, (at + 1) * step)]
            values = values.reshape(-1, LANES)
            turned = jnp.dot(first_v[at, :, : values.shape[0]], values, preferred_element_type=jnp.float32)
            turned = turned.astype(jnp.bfloat16).reshape(n_c, height, LANES)
            sent2[t, :, at * height : (at + 1) * height] = turned
        steps2[t] = exchange(sent2, came2, send_sem2, recv_sem2, self_sem.at[1, t], t, col, n_c, "col")

    lane = lax.broadcasted_iota(jnp.int32, (1, LANES), 1) % width
    cosine = (lane < width // 2) | ((lane == width // 2) & (row == 0))
    load_second.wait()
    out_rows = sent3.shape[2]
    for t in order:
        for copy in steps2[t]:
            copy.wait()
        values = came2[t].reshape(-1, LANES)
        even = jnp.dot(second_v[0], values, preferred_element_type=jnp.float32)
        odd = jnp.dot(second_v[1], values, preferred_element_type=jnp.float32)
        both = jnp.where(cosine, even, odd)
        if t == tiles - 1:
            for r in range(n_r):
                block = packed_rows(both[r * out_rows : (r + 1) * out_rows], parts, used)
                sent3[t, r, 0 : out_rows // parts] = block.astype(jnp.bfloat16)
        else:
            sent3[t] = both.astype(jnp.bfloat16).reshape(sent3.shape[1:])
        steps3[t] = exchange(sent3, came3, send_sem3, recv_sem3, self_sem.at[2, t], t, row, n_r, "row")

    load_back.wait()
    load_wout.wait()
    for t in order:
        lo, hi = spans[t]
        for copy in steps3[t]:
            copy.wait()
        source = came3.at[t]
        if t == tiles - 1:
            size = out_rows // parts
            for p, block in enumerate(widened(came3[t, :, 0:size], parts, used)):
                wide3_v[:, p * size : (p + 1) * size] = block
            source = wide3_v
        total = jnp.dot(source[0], back_v[0, :, : hi - lo], preferred_element_type=jnp.float32)
        for r in range(1, n_r):
            total = total + jnp.dot(source[r], back_v[r, :, : hi - lo], preferred_element_type=jnp.float32)
        share = jnp.dot(total.astype(jnp.bfloat16), wout_v[lo:hi, :], preferred_element_type=jnp.float32)
        if t == order[0]:
            acc_v[...] = share
        elif t != order[-1]:
            acc_v[...] += share
        else:
            out[...] = (acc_v[...] + share).reshape(out.shape).astype(jnp.bfloat16)


def fused_shards(n_r, n_c, tokens, norm_gain, w_in, w_out):
    rows_first, rows_second, features = tokens.shape
    channels = w_in.shape[1]
    length_first = rows_first * n_r
    block = length_first // n_c
    chunk = SUBLANES // block
    chunks = -(-rows_second // chunk)
    padded = chunks * SUBLANES
    groups = channels // GROUP
    tiles = -(-groups // n_r)
    rows = rows_first * rows_second
    length_second = rows_second * n_c
    out_rows = length_second // n_r * block
    forward, back = channel_tables(n_r)
    first, second = position_tables(rows_first, rows_second, n_r, n_c, chunk, chunks)
    used = (groups - (tiles - 1) * n_r) * (GROUP // n_r)
    parts = max(p for p in range(1, LANES // used + 1) if rows % (SUBLANES * p) == 0 and out_rows % (SUBLANES * p) == 0)
    tokens = tokens.transpose(1, 0, 2).reshape(rows, features)
    kind = jnp.bfloat16
    tables = [jnp.asarray(np.asarray(x, np.float32).astype(kind)) for x in (forward, first, second, back)]
    anywhere = pl.BlockSpec(memory_space=pl.ANY)
    vmem = pl.BlockSpec(memory_space=pltpu.VMEM)
    dma = pltpu.SemaphoreType.DMA
    out = pl.pallas_call(
        functools.partial(kernel, n_r, n_c, parts),
        out_shape=jax.ShapeDtypeStruct((length_second // n_r, block, features), kind),
        in_specs=[anywhere, vmem] + [anywhere] * 6,
        out_specs=vmem,
        scratch_shapes=[
            pltpu.VMEM(tokens.shape, kind),
            pltpu.VMEM((rows, features), kind),
            pltpu.VMEM(w_in.shape, kind),
            pltpu.VMEM(w_out.shape, kind),
            pltpu.VMEM(forward.shape, kind),
            pltpu.VMEM(first.shape[1:], kind),
            pltpu.VMEM(second.shape[1:], kind),
            pltpu.VMEM(back.shape, kind),
            pltpu.VMEM((tiles, n_r, rows, LANES), kind),
            pltpu.VMEM((tiles, n_r, rows, LANES), kind),
            pltpu.VMEM((tiles, n_c, padded, LANES), kind),
            pltpu.VMEM((tiles, n_c, padded, LANES), kind),
            pltpu.VMEM((tiles, n_r, out_rows, LANES), kind),
            pltpu.VMEM((tiles, n_r, out_rows, LANES), kind),
            pltpu.VMEM((n_r, rows, LANES), kind),
            pltpu.VMEM((n_r, out_rows, LANES), kind),
            pltpu.VMEM((out_rows, features), jnp.float32),
            dma((6 + tiles,)),
            dma((3, tiles)),
            dma((tiles, n_r)),
            dma((tiles, n_r)),
            dma((tiles, n_c)),
            dma((tiles, n_c)),
            dma((tiles, n_r)),
            dma((tiles, n_r)),
        ],
        compiler_params=pltpu.CompilerParams(
            collective_id=0, has_side_effects=True, vmem_limit_bytes=60 * 1024 * 1024
        ),
    )(tokens, norm_gain.reshape(-1, LANES), w_in, w_out, *tables)
    return out


def fits(n_r, n_c, tokens_shape, channels):
    length_first, length_second, _ = tokens_shape
    rows = length_first // n_r * (length_second // n_c)
    out_rows = length_second // n_r * (length_first // n_c)
    return (
        GROUP % (2 * n_r) == 0
        and length_first % (2 * n_c) == 0
        and SUBLANES % (length_first // n_c) == 0
        and rows % SUBLANES == 0
        and out_rows % SUBLANES == 0
        and length_first // n_r * (SUBLANES // (length_first // n_c)) % SUBLANES == 0
        and length_second % n_r == 0
    )


def tables(length):
    series = jnp.arange(length, dtype=jnp.int32)
    product = series[:, None] * series[None, :] % length
    angles = product.astype(jnp.float32) * (2.0 * math.pi / length)
    return (jnp.cos(angles), jnp.sin(angles))


def folded_order(length_first, devices):
    block = length_first // devices
    half_block = block // 2
    series = jnp.arange(length_first, dtype=jnp.int32)
    device = series // block
    inner = series % block
    lower = device * half_block + inner
    upper = length_first - device * half_block - (inner - half_block)
    upper = jnp.where((device == 0) & (inner == half_block), length_first // 2, upper)
    return jnp.where(inner < half_block, lower, upper) % length_first


def to_channels(values, row_count):
    rows_first, rows_second, channels = values.shape
    width = channels // row_count
    parted = values.reshape(rows_first, rows_second, row_count, width).transpose(2, 0, 1, 3)
    return parted.reshape(row_count * rows_first, rows_second * width)


def product(table, values):
    return jnp.dot(table, values, precision=highest)


def middle(real_part, imag_part, width):
    length_first = real_part.shape[0]
    rows_second = real_part.shape[1] // width
    col_count = lax.axis_size("col")
    length_second = rows_second * col_count
    positions = length_first * length_second
    frequency = folded_order(length_first, col_count)
    series = jnp.arange(length_first, dtype=jnp.int32)
    first_angle = (frequency[:, None] * series[None, :] % length_first).astype(jnp.float32)
    first_angle = first_angle * (2.0 * math.pi / length_first)
    first_cos = jnp.cos(first_angle)
    first_sin = jnp.sin(first_angle)
    first_real = product(first_cos, real_part)
    first_imag = -product(first_sin, real_part)
    first_real = first_real + product(first_sin, imag_part)
    first_imag = first_imag + product(first_cos, imag_part)
    first_real = first_real.reshape(length_first, rows_second, width)
    first_imag = first_imag.reshape(length_first, rows_second, width)
    second_index = lax.axis_index("col") * rows_second + jnp.arange(rows_second, dtype=jnp.int32)
    twiddle_angle = (frequency[:, None] * second_index[None, :] % positions).astype(jnp.float32)
    twiddle_angle = twiddle_angle * (2.0 * math.pi / positions)
    twiddle_cos = jnp.cos(twiddle_angle)[:, :, None]
    twiddle_sin = jnp.sin(twiddle_angle)[:, :, None]
    turned_real = first_real * twiddle_cos + first_imag * twiddle_sin
    turned_imag = first_imag * twiddle_cos - first_real * twiddle_sin
    turned = jnp.stack([turned_real, turned_imag]).transpose(0, 2, 1, 3)
    turned = turned.reshape(2, rows_second, length_first * width)
    exchanged = lax.all_to_all(
        turned.astype(jnp.bfloat16), "col", split_axis=2, concat_axis=1, tiled=True
    ).astype(turned.dtype)
    second_cos, second_sin = tables(length_second)
    block = length_first // col_count
    out_shape = (length_second, block, width)
    out_real = (product(second_cos, exchanged[0]) + product(second_sin, exchanged[1])).reshape(
        out_shape
    )
    return out_real


def shards(tokens, norm_gain, w_in, w_out):
    rows_first, rows_second, features = tokens.shape
    row_count = lax.axis_size("row")
    length_first = rows_first * row_count
    length_second = rows_second * lax.axis_size("col")
    channels = w_in.shape[1]
    width = channels // row_count
    groups = channels // GROUP
    scaling = 1.0 / math.sqrt(length_first * length_second * GROUP)
    floats = tokens.astype(jnp.float32)
    normed = (
        floats
        * lax.rsqrt(jnp.mean(floats * floats, axis=-1, keepdims=True) + norm_eps)
        * norm_gain.astype(jnp.float32)
    ).astype(jnp.bfloat16)
    mapped = jnp.dot(normed.reshape(-1, features), w_in, preferred_element_type=jnp.float32)
    mapped = mapped.astype(jnp.bfloat16).reshape(rows_first, rows_second, channels)
    channel_cos, channel_sin = tables(GROUP)
    grouped = mapped.astype(jnp.float32).reshape(rows_first, rows_second, groups, GROUP)
    spec_real = jnp.einsum("abgj,jm->abgm", grouped, channel_cos, precision=highest)
    spec_imag = -jnp.einsum("abgj,jm->abgm", grouped, channel_sin, precision=highest)
    stacked = jnp.stack(
        [
            to_channels(spec_real.reshape(rows_first, rows_second, channels), row_count),
            to_channels(spec_imag.reshape(rows_first, rows_second, channels), row_count),
        ]
    )
    arrived = lax.all_to_all(
        stacked.astype(jnp.bfloat16), "row", split_axis=1, concat_axis=1, tiled=True
    ).astype(stacked.dtype)
    result = middle(arrived[0], arrived[1], width)
    spectrum = (result * scaling).astype(jnp.bfloat16)
    returned = lax.all_to_all(spectrum, "row", split_axis=0, concat_axis=2, tiled=True)
    mixed = jnp.dot(returned.reshape(-1, channels), w_out, preferred_element_type=jnp.float32)
    return mixed.astype(jnp.bfloat16).reshape(returned.shape[0], returned.shape[1], features)


def solution(mesh):
    in_specs = (P("row", "col", None), P(), P(), P())
    out_specs = P("row", "col", None)
    n_r, n_c = mesh.shape["row"], mesh.shape["col"]

    def run(tokens, norm_gain, w_in, w_out):
        whole = fits(n_r, n_c, tokens.shape, w_in.shape[1])
        body = functools.partial(fused_shards, n_r, n_c) if whole else shards
        return jax.shard_map(body, mesh=mesh, in_specs=in_specs, out_specs=out_specs, check_vma=False)(
            tokens, norm_gain, w_in, w_out
        )

    return run
```

```python
import functools
import math

import jax
import jax.numpy as jnp
import numpy as np
from jax import lax
from jax.experimental import pallas as pl
from jax.experimental.pallas import tpu as pltpu
from jax.sharding import PartitionSpec as P

GROUP = 128
LANES = 128
SUBLANES = 16
MESH = pl.DeviceIdType.MESH


norm_eps = 1e-06
highest = lax.Precision.HIGHEST


def folded_list(length_first, devices):
    block = length_first // devices
    half = block // 2
    result = np.zeros(length_first, np.int64)
    for device in range(devices):
        for inner in range(block):
            if inner < half:
                value = device * half + inner
            elif device == 0 and inner == half:
                value = length_first // 2
            else:
                value = length_first - device * half - (inner - half)
            result[device * block + inner] = value % length_first
    return result


def channel_tables(row_count):
    width = GROUP // row_count
    half = width // 2
    per_tile = LANES // width
    j = np.arange(GROUP)
    forward = np.zeros((row_count, per_tile * GROUP, LANES))
    back = np.zeros((row_count, LANES, per_tile * GROUP))
    for row in range(row_count):
        for x in range(width):
            m = row * half + x % half
            cosine = x < half
            column = np.cos(2 * np.pi * j * m / GROUP) if cosine else np.sin(2 * np.pi * j * m / GROUP)
            entries = [(m, 1.0)]
            if not cosine and m == 0:
                column = np.cos(np.pi * j)
                entries = [(GROUP // 2, 1.0)]
            elif m:
                entries = [(m, 1.0 if cosine else -1.0), (GROUP - m, 1.0)]
            for g in range(per_tile):
                forward[row, g * GROUP : (g + 1) * GROUP, g * width + x] = column
                for at, sign in entries:
                    back[row, g * width + x, g * GROUP + at] = sign
    return forward, back


def position_tables(rows_first, rows_second, row_count, col_count, chunk, chunks):
    length_first = rows_first * row_count
    length_second = rows_second * col_count
    positions = length_first * length_second
    block = length_first // col_count
    half = block // 2
    a = np.arange(length_first)
    first = np.zeros((col_count, chunks, col_count, block, chunk, row_count, chunk, rows_first))
    for col in range(col_count):
        for i in range(rows_second):
            at, j = divmod(i, chunk)
            p = a * length_second + col * rows_second + i
            for target in range(col_count):
                for f_at in range(half):
                    f = target * half + f_at
                    angle = 2 * np.pi * (f * p % positions) / positions
                    real, imag = np.cos(angle), -np.sin(angle)
                    if f == 0:
                        real, imag = np.ones(length_first), (-1.0) ** a
                    first[col, at, target, 2 * f_at, j, :, j, :] = real.reshape(row_count, rows_first)
                    first[col, at, target, 2 * f_at + 1, j, :, j, :] = imag.reshape(row_count, rows_first)
    first = first.reshape(col_count, chunks, col_count * block * chunk, row_count, chunk * rows_first)
    rest = rows_second - (chunks - 1) * chunk
    last = first[:, -1, :, :, : rest * rows_first].reshape(col_count, col_count * block * chunk, -1)
    first = first.reshape(col_count, chunks, col_count * block * chunk, -1)
    first[:, -1] = 0.0
    first[:, -1, :, : last.shape[-1]] = last
    k_b = np.arange(length_second)
    second = np.zeros((2, 2, length_second, block, col_count, chunks, block, chunk))
    for other in range(2):
        for s in range(block):
            for source in range(col_count):
                for i in range(rows_second):
                    b = source * rows_second + i
                    f_at, upper = s % half, s >= half
                    at, j = divmod(i, chunk)
                    re_at, im_at = (source, at, 2 * f_at, j), (source, at, 2 * f_at + 1, j)
                    if other == 0 and f_at == 0:
                        shift = length_first // 2 if upper else 0
                        angle = 2 * np.pi * (b * (k_b * length_first + shift) % positions) / positions
                        place = im_at if upper else re_at
                        second[(other, 0, slice(None), s) + place] = np.cos(angle)
                        second[(other, 1, slice(None), s) + place] = np.sin(angle)
                        continue
                    sign = -1.0 if upper else 1.0
                    angle = 2 * np.pi * (b * (k_b + (1 if upper else 0)) % length_second) / length_second
                    second[(other, 0, slice(None), s) + re_at] = np.cos(angle)
                    second[(other, 0, slice(None), s) + im_at] = np.sin(angle) * sign
                    second[(other, 1, slice(None), s) + re_at] = np.sin(angle)
                    second[(other, 1, slice(None), s) + im_at] = -np.cos(angle) * sign
    second = second.reshape(2, 2, length_second * block, col_count * chunks * block * chunk)
    return first, second / math.sqrt(positions * GROUP)


def widened(packed, parts, used):
    count, rows, lanes = packed.shape
    flat = packed.reshape(count * rows, lanes).astype(jnp.float32)
    keep = lax.broadcasted_iota(jnp.int32, (1, lanes), 1) < used
    blocks = []
    for p in range(parts):
        block = flat if p == 0 else pltpu.roll(flat, lanes - p * used, 1)
        blocks.append(jnp.where(keep, block, 0.0).astype(packed.dtype).reshape(count, rows, lanes))
    return blocks


def packed_rows(values, parts, used):
    rows = values.shape[0] // parts
    total = values[:rows]
    for p in range(1, parts):
        total = total + pltpu.roll(values[p * rows : (p + 1) * rows], p * used, 1)
    return total


def kernel(
    n_r, n_c, parts, tokens, gain, w_in, forward, first, second, back, out,
    tok_v, norm_v, win_v, forward_v, first_v, second_v, back_v,
    sent1, came1, sent2, came2, sent3, came3, wide_v, wide3_v,
    load_sem, self_sem, send_sem1, recv_sem1, send_sem2, recv_sem2, send_sem3, recv_sem3,
):
    row, col = lax.axis_index("row"), lax.axis_index("col")
    rows, features = tokens.shape
    channels = w_in.shape[1]
    tiles = sent1.shape[0]
    span = n_r * GROUP
    spans = [(t * span, min(channels, (t + 1) * span)) for t in range(tiles)]
    width = GROUP // n_r
    used = (spans[-1][1] - spans[-1][0]) // GROUP * width
    order = [tiles - 1] + list(range(tiles - 1))

    barrier = pltpu.get_barrier_semaphore()
    for d in range(1, n_r):
        pl.semaphore_signal(barrier, inc=1, device_id={"row": lax.rem(row + d, n_r)}, device_id_type=MESH)
    for d in range(1, n_c):
        pl.semaphore_signal(barrier, inc=1, device_id={"col": lax.rem(col + d, n_c)}, device_id_type=MESH)

    load_tok = pltpu.make_async_copy(tokens, tok_v, load_sem.at[0])
    load_tok.start()
    load_win = [
        pltpu.make_async_copy(w_in.at[:, lo:hi], win_v.at[:, lo:hi], load_sem.at[6 + t])
        for t, (lo, hi) in enumerate(spans)
    ]
    load_forward = pltpu.make_async_copy(forward, forward_v, load_sem.at[1])
    load_first = pltpu.make_async_copy(first.at[col], first_v, load_sem.at[2])
    load_second = pltpu.make_async_copy(second.at[jnp.minimum(col, 1)], second_v, load_sem.at[3])
    load_back = pltpu.make_async_copy(back, back_v, load_sem.at[4])
    load_win[order[0]].start()
    load_forward.start()
    for t in order[1:]:
        load_win[t].start()
    load_first.start()
    load_second.start()

    load_tok.wait()
    floats = tok_v[...].astype(jnp.float32)
    inverse = lax.rsqrt(jnp.mean(floats * floats, axis=-1, keepdims=True) + norm_eps)
    gains = gain[...].astype(jnp.float32)
    for at in range(features // LANES):
        lanes = slice(at * LANES, (at + 1) * LANES)
        scaled = tok_v[:, lanes].astype(jnp.float32) * inverse * gains[at : at + 1, :]
        norm_v[:, lanes] = scaled.astype(jnp.bfloat16)

    def exchange(sent, came, send_sem, recv_sem, self_sem_at, t, me, count, axis):
        size = sent.shape[2]
        if axis == "row" and t == tiles - 1:
            size = size // parts
        own = pltpu.make_async_copy(sent.at[t, me, 0:size], came.at[t, me, 0:size], self_sem_at)
        copies = []
        for d in sorted(range(1, count), key=lambda d: -min(d, count - d)):
            target = lax.rem(me + d, count)
            copy = pltpu.make_async_remote_copy(
                src_ref=sent.at[t, target, 0:size],
                dst_ref=came.at[t, me, 0:size],
                send_sem=send_sem.at[t, d],
                recv_sem=recv_sem.at[t, d],
                device_id={axis: target},
                device_id_type=MESH,
            )
            copy.start()
            copies.append(copy)
        own.start()
        return [own] + copies

    steps1, steps2, steps3 = {}, {}, {}
    for t in order:
        lo, hi = spans[t]
        load_win[t].wait()
        mapped = jnp.dot(norm_v[...], win_v[:, lo:hi], preferred_element_type=jnp.float32).astype(jnp.bfloat16)
        if t == order[0]:
            load_forward.wait()
        for r in range(n_r):
            piece = jnp.dot(mapped, forward_v[r, : hi - lo, :], preferred_element_type=jnp.float32)
            if t == tiles - 1:
                sent1[t, r, 0 : rows // parts] = packed_rows(piece, parts, used).astype(jnp.bfloat16)
            else:
                sent1[t, r] = piece.astype(jnp.bfloat16)
        if t == order[0]:
            pl.semaphore_wait(barrier, n_r + n_c - 2)
        steps1[t] = exchange(sent1, came1, send_sem1, recv_sem1, self_sem.at[0, t], t, row, n_r, "row")

    load_back.start()
    load_first.wait()
    chunks, high, depth = first_v.shape
    step = depth // n_r
    height = high // n_c
    for t in order:
        for copy in steps1[t]:
            copy.wait()
        source = came1.at[t]
        if t == tiles - 1:
            size = rows // parts
            for p, block in enumerate(widened(came1[t, :, 0:size], parts, used)):
                wide_v[:, p * size : (p + 1) * size] = block
            source = wide_v
        for at in range(chunks):
            values = source[:, at * step : min(rows, (at + 1) * step)]
            values = values.reshape(-1, LANES)
            turned = jnp.dot(first_v[at, :, : values.shape[0]], values, preferred_element_type=jnp.float32)
            turned = turned.astype(jnp.bfloat16).reshape(n_c, height, LANES)
            sent2[t, :, at * height : (at + 1) * height] = turned
        steps2[t] = exchange(sent2, came2, send_sem2, recv_sem2, self_sem.at[1, t], t, col, n_c, "col")

    lane = lax.broadcasted_iota(jnp.int32, (1, LANES), 1) % width
    cosine = (lane < width // 2) | ((lane == width // 2) & (row == 0))
    load_second.wait()
    out_rows = sent3.shape[2]
    for t in order:
        for copy in steps2[t]:
            copy.wait()
        values = came2[t].reshape(-1, LANES)
        even = jnp.dot(second_v[0], values, preferred_element_type=jnp.float32)
        odd = jnp.dot(second_v[1], values, preferred_element_type=jnp.float32)
        both = jnp.where(cosine, even, odd)
        if t == tiles - 1:
            for r in range(n_r):
                block = packed_rows(both[r * out_rows : (r + 1) * out_rows], parts, used)
                sent3[t, r, 0 : out_rows // parts] = block.astype(jnp.bfloat16)
        else:
            sent3[t] = both.astype(jnp.bfloat16).reshape(sent3.shape[1:])
        steps3[t] = exchange(sent3, came3, send_sem3, recv_sem3, self_sem.at[2, t], t, row, n_r, "row")

    load_back.wait()
    for t in order:
        lo, hi = spans[t]
        for copy in steps3[t]:
            copy.wait()
        source = came3.at[t]
        if t == tiles - 1:
            size = out_rows // parts
            for p, block in enumerate(widened(came3[t, :, 0:size], parts, used)):
                wide3_v[:, p * size : (p + 1) * size] = block
            source = wide3_v
        total = jnp.dot(source[0], back_v[0, :, : hi - lo], preferred_element_type=jnp.float32)
        for r in range(1, n_r):
            total = total + jnp.dot(source[r], back_v[r, :, : hi - lo], preferred_element_type=jnp.float32)
        out[:, lo:hi] = total.astype(jnp.bfloat16)


def last_product(spectrum, w_out, out):
    total = jnp.dot(spectrum[...], w_out[...], preferred_element_type=jnp.float32)
    out[...] = total.reshape(out.shape).astype(jnp.bfloat16)


def fused_shards(n_r, n_c, tokens, norm_gain, w_in, w_out):
    rows_first, rows_second, features = tokens.shape
    channels = w_in.shape[1]
    length_first = rows_first * n_r
    block = length_first // n_c
    chunk = SUBLANES // block
    chunks = -(-rows_second // chunk)
    padded = chunks * SUBLANES
    groups = channels // GROUP
    tiles = -(-groups // n_r)
    rows = rows_first * rows_second
    length_second = rows_second * n_c
    out_rows = length_second // n_r * block
    forward, back = channel_tables(n_r)
    first, second = position_tables(rows_first, rows_second, n_r, n_c, chunk, chunks)
    used = (groups - (tiles - 1) * n_r) * (GROUP // n_r)
    parts = max(p for p in range(1, LANES // used + 1) if rows % (SUBLANES * p) == 0 and out_rows % (SUBLANES * p) == 0)
    tokens = tokens.transpose(1, 0, 2).reshape(rows, features)
    kind = jnp.bfloat16
    tables = [jnp.asarray(np.asarray(x, np.float32).astype(kind)) for x in (forward, first, second, back)]
    anywhere = pl.BlockSpec(memory_space=pl.ANY)
    vmem = pl.BlockSpec(memory_space=pltpu.VMEM)
    dma = pltpu.SemaphoreType.DMA
    spectrum = pl.pallas_call(
        functools.partial(kernel, n_r, n_c, parts),
        out_shape=jax.ShapeDtypeStruct((out_rows, channels), kind),
        in_specs=[anywhere, vmem] + [anywhere] * 5,
        out_specs=vmem,
        scratch_shapes=[
            pltpu.VMEM(tokens.shape, kind),
            pltpu.VMEM((rows, features), kind),
            pltpu.VMEM(w_in.shape, kind),
            pltpu.VMEM(forward.shape, kind),
            pltpu.VMEM(first.shape[1:], kind),
            pltpu.VMEM(second.shape[1:], kind),
            pltpu.VMEM(back.shape, kind),
            pltpu.VMEM((tiles, n_r, rows, LANES), kind),
            pltpu.VMEM((tiles, n_r, rows, LANES), kind),
            pltpu.VMEM((tiles, n_c, padded, LANES), kind),
            pltpu.VMEM((tiles, n_c, padded, LANES), kind),
            pltpu.VMEM((tiles, n_r, out_rows, LANES), kind),
            pltpu.VMEM((tiles, n_r, out_rows, LANES), kind),
            pltpu.VMEM((n_r, rows, LANES), kind),
            pltpu.VMEM((n_r, out_rows, LANES), kind),
            dma((6 + tiles,)),
            dma((3, tiles)),
            dma((tiles, n_r)),
            dma((tiles, n_r)),
            dma((tiles, n_c)),
            dma((tiles, n_c)),
            dma((tiles, n_r)),
            dma((tiles, n_r)),
        ],
        compiler_params=pltpu.CompilerParams(
            collective_id=0, has_side_effects=True, vmem_limit_bytes=53 * 1024 * 1024
        ),
    )(tokens, norm_gain.reshape(-1, LANES), w_in, *tables)
    return pl.pallas_call(
        last_product,
        out_shape=jax.ShapeDtypeStruct((length_second // n_r, block, features), kind),
        in_specs=[vmem] * 2,
        out_specs=vmem,
        compiler_params=pltpu.CompilerParams(vmem_limit_bytes=16 * 1024 * 1024),
    )(spectrum, w_out)


def fits(n_r, n_c, tokens_shape, channels):
    length_first, length_second, _ = tokens_shape
    rows = length_first // n_r * (length_second // n_c)
    out_rows = length_second // n_r * (length_first // n_c)
    return (
        GROUP % (2 * n_r) == 0
        and length_first % (2 * n_c) == 0
        and SUBLANES % (length_first // n_c) == 0
        and rows % SUBLANES == 0
        and out_rows % SUBLANES == 0
        and length_first // n_r * (SUBLANES // (length_first // n_c)) % SUBLANES == 0
        and length_second % n_r == 0
    )


def tables(length):
    series = jnp.arange(length, dtype=jnp.int32)
    product = series[:, None] * series[None, :] % length
    angles = product.astype(jnp.float32) * (2.0 * math.pi / length)
    return (jnp.cos(angles), jnp.sin(angles))


def folded_order(length_first, devices):
    block = length_first // devices
    half_block = block // 2
    series = jnp.arange(length_first, dtype=jnp.int32)
    device = series // block
    inner = series % block
    lower = device * half_block + inner
    upper = length_first - device * half_block - (inner - half_block)
    upper = jnp.where((device == 0) & (inner == half_block), length_first // 2, upper)
    return jnp.where(inner < half_block, lower, upper) % length_first


def to_channels(values, row_count):
    rows_first, rows_second, channels = values.shape
    width = channels // row_count
    parted = values.reshape(rows_first, rows_second, row_count, width).transpose(2, 0, 1, 3)
    return parted.reshape(row_count * rows_first, rows_second * width)


def product(table, values):
    return jnp.dot(table, values, precision=highest)


def middle(real_part, imag_part, width):
    length_first = real_part.shape[0]
    rows_second = real_part.shape[1] // width
    col_count = lax.axis_size("col")
    length_second = rows_second * col_count
    positions = length_first * length_second
    frequency = folded_order(length_first, col_count)
    series = jnp.arange(length_first, dtype=jnp.int32)
    first_angle = (frequency[:, None] * series[None, :] % length_first).astype(jnp.float32)
    first_angle = first_angle * (2.0 * math.pi / length_first)
    first_cos = jnp.cos(first_angle)
    first_sin = jnp.sin(first_angle)
    first_real = product(first_cos, real_part)
    first_imag = -product(first_sin, real_part)
    first_real = first_real + product(first_sin, imag_part)
    first_imag = first_imag + product(first_cos, imag_part)
    first_real = first_real.reshape(length_first, rows_second, width)
    first_imag = first_imag.reshape(length_first, rows_second, width)
    second_index = lax.axis_index("col") * rows_second + jnp.arange(rows_second, dtype=jnp.int32)
    twiddle_angle = (frequency[:, None] * second_index[None, :] % positions).astype(jnp.float32)
    twiddle_angle = twiddle_angle * (2.0 * math.pi / positions)
    twiddle_cos = jnp.cos(twiddle_angle)[:, :, None]
    twiddle_sin = jnp.sin(twiddle_angle)[:, :, None]
    turned_real = first_real * twiddle_cos + first_imag * twiddle_sin
    turned_imag = first_imag * twiddle_cos - first_real * twiddle_sin
    turned = jnp.stack([turned_real, turned_imag]).transpose(0, 2, 1, 3)
    turned = turned.reshape(2, rows_second, length_first * width)
    exchanged = lax.all_to_all(
        turned.astype(jnp.bfloat16), "col", split_axis=2, concat_axis=1, tiled=True
    ).astype(turned.dtype)
    second_cos, second_sin = tables(length_second)
    block = length_first // col_count
    out_shape = (length_second, block, width)
    out_real = (product(second_cos, exchanged[0]) + product(second_sin, exchanged[1])).reshape(
        out_shape
    )
    return out_real


def shards(tokens, norm_gain, w_in, w_out):
    rows_first, rows_second, features = tokens.shape
    row_count = lax.axis_size("row")
    length_first = rows_first * row_count
    length_second = rows_second * lax.axis_size("col")
    channels = w_in.shape[1]
    width = channels // row_count
    groups = channels // GROUP
    scaling = 1.0 / math.sqrt(length_first * length_second * GROUP)
    floats = tokens.astype(jnp.float32)
    normed = (
        floats
        * lax.rsqrt(jnp.mean(floats * floats, axis=-1, keepdims=True) + norm_eps)
        * norm_gain.astype(jnp.float32)
    ).astype(jnp.bfloat16)
    mapped = jnp.dot(normed.reshape(-1, features), w_in, preferred_element_type=jnp.float32)
    mapped = mapped.astype(jnp.bfloat16).reshape(rows_first, rows_second, channels)
    channel_cos, channel_sin = tables(GROUP)
    grouped = mapped.astype(jnp.float32).reshape(rows_first, rows_second, groups, GROUP)
    spec_real = jnp.einsum("abgj,jm->abgm", grouped, channel_cos, precision=highest)
    spec_imag = -jnp.einsum("abgj,jm->abgm", grouped, channel_sin, precision=highest)
    stacked = jnp.stack(
        [
            to_channels(spec_real.reshape(rows_first, rows_second, channels), row_count),
            to_channels(spec_imag.reshape(rows_first, rows_second, channels), row_count),
        ]
    )
    arrived = lax.all_to_all(
        stacked.astype(jnp.bfloat16), "row", split_axis=1, concat_axis=1, tiled=True
    ).astype(stacked.dtype)
    result = middle(arrived[0], arrived[1], width)
    spectrum = (result * scaling).astype(jnp.bfloat16)
    returned = lax.all_to_all(spectrum, "row", split_axis=0, concat_axis=2, tiled=True)
    mixed = jnp.dot(returned.reshape(-1, channels), w_out, preferred_element_type=jnp.float32)
    return mixed.astype(jnp.bfloat16).reshape(returned.shape[0], returned.shape[1], features)


def solution(mesh):
    in_specs = (P("row", "col", None), P(), P(), P())
    out_specs = P("row", "col", None)
    n_r, n_c = mesh.shape["row"], mesh.shape["col"]

    def run(tokens, norm_gain, w_in, w_out):
        whole = fits(n_r, n_c, tokens.shape, w_in.shape[1])
        body = functools.partial(fused_shards, n_r, n_c) if whole else shards
        return jax.shard_map(body, mesh=mesh, in_specs=in_specs, out_specs=out_specs, check_vma=False)(
            tokens, norm_gain, w_in, w_out
        )

    return run
```
